32 devices in a mesh: fs: 16 (over z, y, x), tp: 2 (over core).
Axes of the slice: x: 2, y: 2, z: 4, core: 2. Of those that a mesh axis runs over, the one named last changes fastest.
Arguments:
- residual_in: bfloat16 [4096, 2048], P(('fs', 'tp')), may hold values from -6 to 6
- gain_first: float32 [2048], replicated, may hold values from 0.1 to 1.9
- gain_mixer: float32 [2048], replicated, may hold values from 0.1 to 1.9
- gain_second: float32 [2048], replicated, may hold values from 0.1 to 1.9
- gate_weight: float32 [2048, 6144], P('fs', 'tp'), may hold values from -0.125 to 0.125
- gate_scale: float32 [6144], P('tp'), may hold values from 0.3 to 3
- up_weight: float32 [2048, 6144], P('fs', 'tp'), may hold values from -0.125 to 0.125
- up_scale: float32 [6144], P('tp'), may hold values from 0.3 to 3
- down_weight: float32 [6144, 2048], P('tp', 'fs'), may hold values from -0.078125 to 0.078125
- down_scale: float32 [2048], P('fs'), may hold values from 0.3 to 3
- query_weight: float32 [2048, 2048], P('fs', 'tp'), may hold values from -0.125 to 0.125
- query_scale: float32 [2048], P('tp'), may hold values from 0.3 to 3
- key_weight: float32 [2048, 2048], P('fs', 'tp'), may hold values from -0.125 to 0.125
- key_scale: float32 [2048], P('tp'), may hold values from 0.3 to 3
- value_weight: float32 [2048, 2048], P('fs', 'tp'), may hold values from -0.125 to 0.125
- value_scale: float32 [2048], P('tp'), may hold values from 0.3 to 3
- output_weight: float32 [2048, 2048], P('tp', 'fs'), may hold values from -0.125 to 0.125
- output_scale: float32 [2048], P('fs'), may hold values from 0.3 to 3
Outputs:
- residual_out: bfloat16 [4096, 2048], P(('fs', 'tp'))
The draws below stay inside these ranges and needn't reach their ends.
All inputs are finite; a program needn't handle non-finite values.
Results may differ from the reference program's by a relative error of at most 0.028.
Values may be sent and summed in bfloat16 or wider, within the bound.
A program may use at most 128 MiB of HBM per device.

```python
import math
import jax
import jax.numpy as jnp
from jax import lax

D = 2048
FF = 6144
HEADS = 8
HEAD_DIM = 256
MIX_WIDTH = 2048
TOK = 256
BLOCK = 64
TOKENS = 4096
N_FS = 16
N_TP = 2


def steps_of(stream_key, dims, shards, low, top_value):
    loudness, own = 1.0, jax.random.fold_in(stream_key, 6)
    for axis_at, parts in shards:
        draws = jnp.exp(jax.random.uniform(jax.random.fold_in(own, axis_at), (parts,), jnp.float32, low / len(shards), top_value / len(shards)))
        loudness = loudness * jnp.repeat(draws, dims[axis_at] // parts).reshape([-1 if axis == axis_at else 1 for axis in range(len(dims))])
    return loudness


def centred(stream_key, extent, scale, reach, split=(), kind=jnp.bfloat16):
    entries = scale * jax.random.normal(stream_key, extent, jnp.float32)
    if split:
        entries = entries * steps_of(stream_key, extent, split, -0.22, 0.18)
    return jnp.clip(entries, -reach, reach).astype(kind)


def setup_inputs(seed: int = 0) -> dict:
    key_list = jax.random.split(jax.random.key(seed), 19)
    residual_in = centred(key_list[0], (TOKENS, D), 1.0, 6.0, ((0, 32),))
    gain_first = jnp.clip(1.0 + 0.18 * jax.random.normal(key_list[1], (D,), jnp.float32), 0.1, 1.9)
    gain_mixer = jnp.clip(1.0 + 0.18 * jax.random.normal(key_list[2], (D,), jnp.float32), 0.1, 1.9)
    gain_second = jnp.clip(1.0 + 0.18 * jax.random.normal(key_list[3], (D,), jnp.float32), 0.1, 1.9)
    gate_weight = centred(key_list[4], (D, FF), D ** -0.5, 0.125, ((0, 16), (1, 2)), jnp.float32)
    gate_scale = jnp.clip(jnp.exp(math.log(3.0) - 2.3025851 * jax.random.uniform(key_list[5], (FF,), jnp.float32) ** steps_of(key_list[5], (FF,), ((0, 2),), -0.2, 0.2)), 0.3, 3.0)
    up_weight = centred(key_list[6], (D, FF), D ** -0.5, 0.125, ((0, 16), (1, 2)), jnp.float32)
    up_scale = jnp.clip(jnp.exp(math.log(3.0) - 2.3025851 * jax.random.uniform(key_list[7], (FF,), jnp.float32) ** steps_of(key_list[7], (FF,), ((0, 2),), -0.2, 0.2)), 0.3, 3.0)
    down_weight = centred(key_list[8], (FF, D), FF ** -0.5, 0.078125, ((0, 2), (1, 16)), jnp.float32)
    down_scale = jnp.clip(jnp.exp(math.log(3.0) - 2.3025851 * jax.random.uniform(key_list[9], (D,), jnp.float32) ** steps_of(key_list[9], (D,), ((0, 16),), -0.2, 0.2)), 0.3, 3.0)
    query_weight = centred(key_list[10], (D, MIX_WIDTH), D ** -0.5, 0.125, ((0, 16), (1, 2)), jnp.float32)
    query_scale = jnp.clip(jnp.exp(math.log(3.0) - 2.3025851 * jax.random.uniform(key_list[11], (MIX_WIDTH,), jnp.float32) ** steps_of(key_list[11], (MIX_WIDTH,), ((0, 2),), -0.2, 0.2)), 0.3, 3.0)
    key_weight = centred(key_list[12], (D, MIX_WIDTH), D ** -0.5, 0.125, ((0, 16), (1, 2)), jnp.float32)
    key_scale = jnp.clip(jnp.exp(math.log(3.0) - 2.3025851 * jax.random.uniform(key_list[13], (MIX_WIDTH,), jnp.float32) ** steps_of(key_list[13], (MIX_WIDTH,), ((0, 2),), -0.2, 0.2)), 0.3, 3.0)
    value_weight = centred(key_list[14], (D, MIX_WIDTH), D ** -0.5, 0.125, ((0, 16), (1, 2)), jnp.float32)
    value_scale = jnp.clip(jnp.exp(math.log(3.0) - 2.3025851 * jax.random.uniform(key_list[15], (MIX_WIDTH,), jnp.float32) ** steps_of(key_list[15], (MIX_WIDTH,), ((0, 2),), -0.2, 0.2)), 0.3, 3.0)
    output_weight = centred(key_list[16], (MIX_WIDTH, D), MIX_WIDTH ** -0.5, 0.125, ((0, 2), (1, 16)), jnp.float32)
    output_scale = jnp.clip(jnp.exp(math.log(3.0) - 2.3025851 * jax.random.uniform(key_list[17], (D,), jnp.float32) ** steps_of(key_list[17], (D,), ((0, 16),), -0.2, 0.2)), 0.3, 3.0)
    return dict(residual_in=residual_in, gain_first=gain_first, gain_mixer=gain_mixer, gain_second=gain_second, gate_weight=gate_weight, gate_scale=gate_scale, up_weight=up_weight, up_scale=up_scale, down_weight=down_weight, down_scale=down_scale, query_weight=query_weight, query_scale=query_scale, key_weight=key_weight, key_scale=key_scale, value_weight=value_weight, value_scale=value_scale, output_weight=output_weight, output_scale=output_scale)


EPSILON = 1e-06
HEAD_FLOOR = 0.25
ROTARY_BASE = 10000.0
HIGHEST = lax.Precision.HIGHEST

def normalize(sequence_rows, gain_vector):
    values = sequence_rows.astype(jnp.float32)
    scaled = values * lax.rsqrt(lax.optimization_barrier(jnp.mean(values * values, axis=-1, keepdims=True)) + EPSILON)
    return (scaled * gain_vector).astype(jnp.bfloat16)

def head_rates(first_head, head_count, length):
    head_number = (first_head + jnp.arange(head_count)).astype(jnp.float32)
    return jnp.exp(jnp.log(1.0 / 16.0) + head_number / (HEADS - 1) * jnp.log(4.0 / length))

def rotate(values, positions):
    half_width = values.shape[-1] // 2
    frequency = ROTARY_BASE ** (-jnp.arange(half_width, dtype=jnp.float32) * 2.0 / values.shape[-1])
    angles = positions[:, None] * frequency[None, :]
    cosine = jnp.cos(angles)[:, None, :]
    sine_value = jnp.sin(angles)[:, None, :]
    front_half = values[..., :half_width]
    back_half = values[..., half_width:]
    return jnp.concatenate([front_half * cosine - back_half * sine_value, back_half * cosine + front_half * sine_value], axis=-1)

def retention(query_pre, key_pre, value_pre, decay_rates):
    length, head_count, head_width = query_pre.shape
    positions = jnp.arange(length, dtype=jnp.float32)
    query_rot = rotate(query_pre, positions).astype(jnp.bfloat16)
    key_rot = rotate(key_pre, positions).astype(jnp.bfloat16)
    value_low = value_pre.astype(jnp.bfloat16)
    blocks = length // BLOCK
    inside = jnp.arange(BLOCK, dtype=jnp.float32)
    distance = inside[:, None] - inside[None, :]
    within = jnp.where(distance >= 0, jnp.exp(-decay_rates[:, None, None] * jnp.maximum(distance, 0.0)), 0.0) * head_width ** (-0.5)
    query_blocks = query_rot.reshape(blocks, BLOCK, head_count, head_width)
    key_blocks = key_rot.reshape(blocks, BLOCK, head_count, head_width)
    value_blocks = value_low.reshape(blocks, BLOCK, head_count, head_width)
    scores = jnp.einsum('nihe,njhe->nhij', query_blocks.astype(jnp.float32), key_blocks.astype(jnp.float32), precision=HIGHEST)
    weights = (scores * within[None]).astype(jnp.bfloat16)
    inner_part = jnp.einsum('nhij,njhe->nihe', weights.astype(jnp.float32), value_blocks.astype(jnp.float32), precision=HIGHEST)
    fading = jnp.exp(-decay_rates[None, :] * (BLOCK - 1.0 - inside[:, None])) * head_width ** (-0.5)
    key_faded = key_blocks.astype(jnp.float32) * fading[None, :, :, None]
    updates = jnp.einsum('njhd,njhe->nhde', key_faded, value_blocks.astype(jnp.float32), precision=HIGHEST)
    block_decay = jnp.exp(-decay_rates * BLOCK)

    def advance(memory_state, update):
        return (memory_state * block_decay[:, None, None] + update, memory_state)
    _, before = lax.scan(advance, jnp.zeros((head_count, head_width, head_width), jnp.float32), updates)
    rising = jnp.exp(-decay_rates[None, :] * (inside[:, None] + 1.0))
    queried = query_blocks.astype(jnp.float32) * rising[None, :, :, None]
    carried_part = jnp.einsum('nihd,nhde->nihe', queried, before, precision=HIGHEST)
    combined = (inner_part + carried_part).reshape(length, head_count, head_width)
    normed = combined * lax.rsqrt(jnp.maximum(lax.optimization_barrier(jnp.mean(combined * combined, axis=-1, keepdims=True)), HEAD_FLOOR))
    return normed.astype(jnp.bfloat16).reshape(length, head_count * head_width)

def partial_sums(inputs, weight, factor, range_width):
    combined = jnp.zeros((inputs.shape[0], weight.shape[1]), jnp.float32)
    for member in range(N_TP):
        partial_piece = jnp.dot(inputs[:, member * range_width:(member + 1) * range_width], weight[member * range_width:(member + 1) * range_width], preferred_element_type=jnp.float32) * factor
        combined = combined + lax.optimization_barrier(partial_piece.astype(jnp.bfloat16)).astype(jnp.float32)
    return combined

def reference(residual_in, gain_first, gain_mixer, gain_second, gate_weight, gate_scale, up_weight, up_scale, down_weight, down_scale, query_weight, query_scale, key_weight, key_scale, value_weight, value_scale, output_weight, output_scale):
    gate_low = gate_weight.astype(jnp.bfloat16)
    up_low = up_weight.astype(jnp.bfloat16)
    down_low = down_weight.astype(jnp.bfloat16)
    query_low = query_weight.astype(jnp.bfloat16)
    key_low = key_weight.astype(jnp.bfloat16)
    value_low = value_weight.astype(jnp.bfloat16)
    output_low = output_weight.astype(jnp.bfloat16)
    decay_rates = head_rates(0, HEADS, TOK)

    def feed_forward(sequence_rows, gain_vector):
        normed = normalize(sequence_rows, gain_vector)
        gate_pre = jnp.dot(normed, gate_low, preferred_element_type=jnp.float32) * gate_scale
        up_pre = jnp.dot(normed, up_low, preferred_element_type=jnp.float32) * up_scale
        hidden = (jax.nn.silu(gate_pre) * up_pre).astype(jnp.bfloat16)
        return partial_sums(hidden, down_low, down_scale, FF // N_TP)

    def one_sequence(sequence_rows):
        middle = (sequence_rows.astype(jnp.float32) + 0.5 * feed_forward(sequence_rows, gain_first)).astype(jnp.bfloat16)
        mixer_input = normalize(middle, gain_mixer)
        query_pre = (jnp.dot(mixer_input, query_low, preferred_element_type=jnp.float32) * query_scale).reshape(TOK, HEADS, HEAD_DIM)
        key_pre = (jnp.dot(mixer_input, key_low, preferred_element_type=jnp.float32) * key_scale).reshape(TOK, HEADS, HEAD_DIM)
        value_pre = (jnp.dot(mixer_input, value_low, preferred_element_type=jnp.float32) * value_scale).reshape(TOK, HEADS, HEAD_DIM)
        mixed = retention(query_pre, key_pre, value_pre, decay_rates)
        mixer_out = partial_sums(mixed, output_low, output_scale, HEADS * HEAD_DIM // N_TP)
        second = (middle.astype(jnp.float32) + mixer_out).astype(jnp.bfloat16)
        return (second.astype(jnp.float32) + 0.5 * feed_forward(second, gain_second)).astype(jnp.bfloat16)
    sequences = residual_in.reshape(N_FS, TOK, D)
    return lax.map(one_sequence, sequences).reshape(N_FS * TOK, D)
```

```python
import math

import jax
import jax.numpy as jnp
from jax import lax
from jax.sharding import PartitionSpec as P

HEADS = 8
HEAD_DIM = 256
BLOCK = 64


EPSILON = 1e-06
HEAD_FLOOR = 0.25
ROTARY_BASE = 10000.0
HIGHEST = lax.Precision.HIGHEST


def normalize(sequence_rows, gain_vector):
    values = sequence_rows.astype(jnp.float32)
    scaled = values * lax.rsqrt(jnp.mean(values * values, axis=-1, keepdims=True) + EPSILON)
    return (scaled * gain_vector).astype(jnp.bfloat16)


def head_rates(first_head, head_count, length):
    head_number = (first_head + jnp.arange(head_count)).astype(jnp.float32)
    return jnp.exp(jnp.log(1.0 / 16.0) + head_number / (HEADS - 1) * jnp.log(4.0 / length))


def rotate(values, positions):
    half_width = values.shape[-1] // 2
    frequency = ROTARY_BASE ** (-jnp.arange(half_width, dtype=jnp.float32) * 2.0 / values.shape[-1])
    angles = positions[:, None] * frequency[None, :]
    cosine = jnp.cos(angles)[:, None, :]
    sine_value = jnp.sin(angles)[:, None, :]
    front_half = values[..., :half_width]
    back_half = values[..., half_width:]
    return jnp.concatenate(
        [
            front_half * cosine - back_half * sine_value,
            back_half * cosine + front_half * sine_value,
        ],
        axis=-1,
    )


def retention(query_pre, key_pre, value_pre, decay_rates):
    length, head_count, head_width = query_pre.shape
    positions = jnp.arange(length, dtype=jnp.float32)
    query_rot = rotate(query_pre, positions).astype(jnp.bfloat16)
    key_rot = rotate(key_pre, positions).astype(jnp.bfloat16)
    value_low = value_pre.astype(jnp.bfloat16)
    blocks = length // BLOCK
    inside = jnp.arange(BLOCK, dtype=jnp.float32)
    distance = inside[:, None] - inside[None, :]
    within = jnp.where(
        distance >= 0, jnp.exp(-decay_rates[:, None, None] * jnp.maximum(distance, 0.0)), 0.0
    ) * head_width ** (-0.5)
    query_blocks = query_rot.reshape(blocks, BLOCK, head_count, head_width)
    key_blocks = key_rot.reshape(blocks, BLOCK, head_count, head_width)
    value_blocks = value_low.reshape(blocks, BLOCK, head_count, head_width)
    scores = jnp.einsum(
        "nihe,njhe->nhij", query_blocks, key_blocks, preferred_element_type=jnp.float32
    )
    weights = (scores * within[None]).astype(jnp.bfloat16)
    inner_part = jnp.einsum(
        "nhij,njhe->nihe", weights, value_blocks, preferred_element_type=jnp.float32
    )
    fading = jnp.exp(-decay_rates[None, :] * (BLOCK - 1.0 - inside[:, None])) * head_width ** (-0.5)
    key_faded = key_blocks.astype(jnp.float32) * fading[None, :, :, None]
    updates = jnp.einsum(
        "njhd,njhe->nhde", key_faded, value_blocks.astype(jnp.float32), precision=HIGHEST
    )
    block_decay = jnp.exp(-decay_rates * BLOCK)

    def advance(memory_state, update):
        return (memory_state * block_decay[:, None, None] + update, memory_state)

    _, before = lax.scan(
        advance, jnp.zeros((head_count, head_width, head_width), jnp.float32), updates
    )
    rising = jnp.exp(-decay_rates[None, :] * (inside[:, None] + 1.0))
    queried = query_blocks.astype(jnp.float32) * rising[None, :, :, None]
    carried_part = jnp.einsum("nihd,nhde->nihe", queried, before, precision=HIGHEST)
    combined = (inner_part + carried_part).reshape(length, head_count, head_width)
    normed = combined * lax.rsqrt(
        jnp.maximum(jnp.mean(combined * combined, axis=-1, keepdims=True), HEAD_FLOOR)
    )
    return normed.astype(jnp.bfloat16).reshape(length, head_count * head_width)


def split_three(values):
    high = values.astype(jnp.bfloat16)
    rest = values - high.astype(jnp.float32)
    middle_part = rest.astype(jnp.bfloat16)
    low = (rest - middle_part.astype(jnp.float32)).astype(jnp.bfloat16)
    return [high, middle_part, low]


def make_body(n_fs, n_tp, share):
    spread = n_fs // share
    STRIDED = False
    if STRIDED:
        teams = [[m * spread + r for m in range(share)] for r in range(spread)]
    else:
        teams = [[r * share + m for m in range(share)] for r in range(spread)]
    twins = [[team[m] for team in teams] for m in range(share)]
    row_teams = [[f * n_tp + t for f in team for t in range(n_tp)] for team in teams]

    def my_rank():
        position = lax.axis_index("fs")
        return position // spread if STRIDED else position % share

    def fetch(pieces):
        swapped = lax.all_to_all(
            pieces, "fs", split_axis=0, concat_axis=0, axis_index_groups=teams, tiled=True
        )
        return lax.all_gather(swapped, "fs", axis=0, axis_index_groups=twins, tiled=False)

    def order_features(rows):
        if not STRIDED:
            return rows
        count = rows.shape[0]
        return rows.reshape(count, share, spread, -1).swapaxes(1, 2).reshape(count, -1)

    def collect_rows(rows, gain_vector):
        return lax.all_gather(
            order_features(normalize(rows, gain_vector)),
            ("fs", "tp"),
            axis=0,
            axis_index_groups=row_teams,
            tiled=True,
        )

    def return_rows(inputs, weight, factor):
        term = jnp.dot(inputs, weight, preferred_element_type=jnp.float32) * factor
        return lax.psum_scatter(
            term.astype(jnp.bfloat16),
            ("fs", "tp"),
            scatter_dimension=0,
            axis_index_groups=row_teams,
            tiled=True,
        ).astype(jnp.float32)

    def columns_of(weight):
        low = weight.astype(jnp.bfloat16)
        return low.reshape(low.shape[0], share, -1).swapaxes(0, 1)

    def rows_of(weight):
        low = weight.astype(jnp.bfloat16)
        return low.reshape(share, -1, low.shape[1])

    def own(vector, rank):
        width = vector.shape[0] // share
        return lax.dynamic_slice_in_dim(vector, rank * width, width)

    def body(
        residual_in,
        gain_first,
        gain_mixer,
        gain_second,
        gate_weight,
        gate_scale,
        up_weight,
        up_scale,
        down_weight,
        down_scale,
        query_weight,
        query_scale,
        key_weight,
        key_scale,
        value_weight,
        value_scale,
        output_weight,
        output_scale,
    ):
        rank = my_rank()
        hidden_width = gate_weight.shape[1] // share
        mix_width = query_weight.shape[1] // share
        entry = fetch(jnp.concatenate([columns_of(gate_weight), columns_of(up_weight)], axis=2))
        factors = split_three(down_scale) + split_three(output_scale)
        factors = jnp.stack(factors + [jnp.zeros_like(factors[0])] * 10)
        leave_piece = jnp.concatenate(
            [
                rows_of(down_weight),
                rows_of(output_weight),
                jnp.broadcast_to(factors[None], (share,) + factors.shape),
            ],
            axis=1,
        )
        first_input = collect_rows(residual_in, gain_first)
        leave_piece, entry = lax.optimization_barrier((leave_piece, entry)) if False else (leave_piece, entry)
        leave = fetch(leave_piece)
        project_piece = jnp.concatenate(
            [columns_of(query_weight), columns_of(key_weight), columns_of(value_weight)], axis=2
        )
        project_piece, leave = lax.optimization_barrier((project_piece, leave)) if False else (project_piece, leave)
        project = fetch(project_piece)

        entry = entry.reshape(-1, 2 * hidden_width)
        project = project.reshape(-1, 3 * mix_width)
        if STRIDED:
            leave = leave.swapaxes(0, 1)
        leave = leave.transpose(2, 0, 1, 3).reshape(leave.shape[2], -1)
        down_full = leave[:hidden_width]
        output_full = leave[hidden_width : hidden_width + mix_width]
        parts = leave[hidden_width + mix_width :].astype(jnp.float32)
        down_factor = parts[0] + parts[1] + parts[2]
        output_factor = parts[3] + parts[4] + parts[5]
        gate_own, up_own = own(gate_scale, rank), own(up_scale, rank)

        def half_step(inputs):
            both = jnp.dot(inputs, entry, preferred_element_type=jnp.float32)
            gate_pre = both[:, :hidden_width] * gate_own
            up_pre = both[:, hidden_width:] * up_own
            hidden = (jax.nn.silu(gate_pre) * up_pre).astype(jnp.bfloat16)
            return return_rows(hidden, down_full, down_factor)

        mlp_first = half_step(first_input)
        middle = (residual_in.astype(jnp.float32) + 0.5 * mlp_first).astype(jnp.bfloat16)
        mixer_input = collect_rows(middle, gain_mixer)
        both = jnp.dot(mixer_input, project, preferred_element_type=jnp.float32)
        scale = jnp.concatenate([own(v, rank) for v in (query_scale, key_scale, value_scale)])
        length = residual_in.shape[0] * n_tp
        heads_own = mix_width // HEAD_DIM
        both = (both * scale).reshape(share, length, 3, heads_own, HEAD_DIM)
        first_head = (lax.axis_index("tp") * share + rank) * heads_own
        decay_rates = head_rates(first_head, heads_own, length)
        mixed = jax.vmap(lambda t: retention(t[:, 0], t[:, 1], t[:, 2], decay_rates))(both)
        mixer_out = return_rows(mixed.reshape(share * length, mix_width), output_full, output_factor)
        second = (middle.astype(jnp.float32) + mixer_out).astype(jnp.bfloat16)
        mlp_second = half_step(collect_rows(second, gain_second))
        return (second.astype(jnp.float32) + 0.5 * mlp_second).astype(jnp.bfloat16)

    return body


def solution(mesh):
    n_fs, n_tp = mesh.shape["fs"], mesh.shape["tp"]
    share = math.gcd(math.gcd(HEADS // n_tp, n_fs), 4)
    body = make_body(n_fs, n_tp, share)
    in_specs = (
        P(("fs", "tp"), None),
        P(),
        P(),
        P(),
        P("fs", "tp"),
        P("tp"),
        P("fs", "tp"),
        P("tp"),
        P("tp", "fs"),
        P("fs"),
        P("fs", "tp"),
        P("tp"),
        P("fs", "tp"),
        P("tp"),
        P("fs", "tp"),
        P("tp"),
        P("tp", "fs"),
        P("fs"),
    )
    out_specs = P(("fs", "tp"), None)
    return jax.shard_map(body, mesh=mesh, in_specs=in_specs, out_specs=out_specs, check_vma=False)
```
